32 devices in a mesh: grp: 2 (over y), ep: 4 (over z), tp: 4 (over x, core).
Axes of the slice: x: 2, y: 2, z: 4, core: 2. Of those that a mesh axis runs over, the one named last changes fastest.
Arguments:
- queries: bfloat16 [3072, 1024], P(('grp', 'ep'), 'tp'), parts along dimension 0, may hold values from -6 to 6
- key_values: bfloat16 [3072, 512], P(('grp', 'ep'), 'tp'), parts along dimension 0, may hold values from -6 to 6
- query_gain: float32 [64], replicated, may hold values from 0.5 to 5
- key_gain: float32 [64], replicated, may hold values from 0.5 to 5
- out_weight: bfloat16 [1024, 2048], P('tp'), may hold values from -0.1875 to 0.1875
- second_batch: bfloat16 [4096, 2048], P(('grp', 'ep', 'tp')), parts along dimension 0, may hold values from -6 to 6
- norm_gain: float32 [2048], replicated, may hold values from 0.1 to 1.9
- routes: int32 [4096, 2], P(('grp', 'ep', 'tp')), parts along dimension 0, may hold values from 0 to 7, all different within a row; in each aligned block of 128 rows (0 to 127, 128 to 255, ...) at most 48 rows name the same one
- route_weights: float32 [4096, 2], P(('grp', 'ep', 'tp')), parts along dimension 0, may hold values from 0.2 to 1
- expert_gate: bfloat16 [8, 2048, 1024], P('ep', None, 'tp'), may hold values from -0.125 to 0.125
- expert_up: bfloat16 [8, 2048, 1024], P('ep', None, 'tp'), may hold values from -0.125 to 0.125
- expert_down: bfloat16 [8, 1024, 2048], P('ep', 'tp'), may hold values from -0.1875 to 0.1875
- shared_gate: bfloat16 [2048, 512], P(None, 'tp'), may hold values from -0.125 to 0.125
- shared_up: bfloat16 [2048, 512], P(None, 'tp'), may hold values from -0.125 to 0.125
- shared_down: bfloat16 [512, 2048], P('tp'), may hold values from -0.25 to 0.25
Outputs:
- mixer_out: bfloat16 [3072, 2048], P(('grp', 'ep', 'tp')), parts along dimension 0
- channel_out: bfloat16 [4096, 2048], P(('grp', 'ep', 'tp')), parts along dimension 0
The draws below stay inside these ranges and needn't reach their ends.
There are 2 independent parts, one for each index of `grp`. The reference program is written for one: setup_inputs(seed, part) draws one part's arguments, and reference() takes and returns one part's arrays. A program takes and returns all parts, laid end to end along the dimension named above; an argument that names none is the same for every part. Nothing has to cross between parts.
Inputs may be any that keep to these rules, and one draw needn't show every extreme that they name: `routes`: each row names 2 different experts. Among the rows of one device no expert is named more than 48 times, and in every draw some expert is named exactly 48 times by the rows of some device.
All inputs are finite; a program needn't handle non-finite values.
Results may differ from the reference program's by a relative error of at most 0.015.
The reference program's roundings to bfloat16 on the way count: a program that leaves them out, or rounds other values in their place, can miss the bound.
Values may be sent and summed in bfloat16 or wider, within the bound.
A program may use at most 128 MiB of HBM per device.

```python
import math
import jax
import jax.numpy as jnp
import numpy as np
from jax import lax

D = 2048
HEAD = 64
HQ_DEV = 4
HQ = 16
KV_HEADS = 4
GRID_W = 64
TOK_A = 384
TOKENS_A = 1536
TOK_B = 128
TOKENS_B = 2048
TOP_K = 2
EXPERTS = 8
FE_DEV = 256
EXPERT_HIDDEN = 1024
SH_DEV = 128
SHARED = 512
CAP = 48
N_EP = 4


def draw_base(key):
    keyvals = jnp.clip(jax.random.normal(jax.random.fold_in(key, 71), (TOKENS_A, KV_HEADS, 2 * HEAD), jnp.float32), -6.0, 6.0)
    queries = jnp.clip(jax.random.normal(jax.random.fold_in(key, 72), (TOKENS_A, HQ, HEAD), jnp.float32), -6.0, 6.0)
    return (queries.reshape(TOKENS_A, HQ * HEAD), keyvals.reshape(TOKENS_A, KV_HEADS * 2 * HEAD))


def draw_queries(key, part):
    return draw_base(key)[0].astype(jnp.bfloat16)


def draw_key_values(key, part):
    return draw_base(key)[1].astype(jnp.bfloat16)


def draw_gain_common(key, salt):
    return 1.0 + 0.18 * jnp.clip(jax.random.normal(jax.random.fold_in(key, salt + 1), (HEAD,), jnp.float32), -2.5, 2.5)


def draw_query_gain(key, part):
    return draw_gain_common(key, 81)


def draw_key_gain(key, part):
    return draw_gain_common(key, 91)


def block_scale(own_key, dims, pieces, low, top_value):
    def one(axis_at, shards_of):
        heights = jax.random.uniform(jax.random.fold_in(jax.random.fold_in(own_key, 6), axis_at), (shards_of,), jnp.float32, low / len(pieces), top_value / len(pieces))
        return jnp.repeat(jnp.exp(heights), dims[axis_at] // shards_of).reshape((-1,) + (1,) * (len(dims) - axis_at - 1))

    level = one(*pieces[0])
    for cut in pieces[1:]:
        level = level * one(*cut)
    return level


def assign_block(rng, own, number, rows, amount, top, reach, slope):
    ranking = jax.random.permutation(rng, amount)
    packed, ordinary = shares(amount, rows * top, reach, slope, True), shares(amount, rows * top, reach, slope, False)
    places = jnp.arange(amount)

    def named(lengths, rotation):
        used = int((lengths > 0).sum())
        fixed = max(1, used // 4)
        passed = fixed + (places - fixed + rotation * (used - fixed)) % max(1, amount - fixed)
        return jnp.zeros((amount,), jnp.int32).at[ranking[jnp.where(places < fixed, places, passed)]].set(jnp.asarray(lengths, jnp.int32))

    lengths = jnp.where(number % 4 == 0, named(packed, number // 4), named(ordinary, number - number // 4 - 1))
    mixed = jax.random.permutation(jax.random.fold_in(own, 3), amount)
    source_of, sink = mixed[0:amount // 2 * 2:2], mixed[1:amount // 2 * 2:2]
    room = jnp.minimum(lengths[source_of] - 1, reach - lengths[sink]) // 2
    room = jnp.where((source_of == ranking[0]) | (sink == ranking[0]) | (lengths[sink] == 0), 0, jnp.maximum(room, 0))
    passed = jax.random.randint(jax.random.fold_in(own, 4), (amount // 2,), 0, 1 << 20) % (room + 1)
    lengths = lengths.at[source_of].add(-passed).at[sink].add(passed)
    items = jnp.searchsorted(jnp.cumsum(lengths), jnp.arange(rows * top), side="right").astype(jnp.int32)
    grid = items.reshape(top, rows).T
    grid = grid[jax.random.permutation(jax.random.fold_in(own, 1), rows)]
    rotation = jax.random.randint(jax.random.fold_in(own, 2), (rows, 1), 0, top)
    return jnp.take_along_axis(grid, (jnp.arange(top)[None, :] + rotation) % top, axis=1)


def shares(amount, total, bound, skew, full):
    loads = [(1 << 20) // math.isqrt(rank ** skew) + 1 for rank in range(1, amount + 1)]
    largest = bound if full else min(bound, max(-(-total // amount), total * loads[0] // sum(loads)))
    least = 1 if total - largest >= amount - 1 else 0
    holding, surplus = [largest] + [least] * (amount - 1), total - largest - least * (amount - 1)
    while surplus > 0:
        candidates = [i for i in range(1, amount) if holding[i] < largest] or [i for i in range(1, amount) if holding[i] < bound]
        mass, budget = sum([loads[i] for i in candidates]), surplus
        for i in candidates:
            extra = min(bound - holding[i], max(1, budget * loads[i] // mass), surplus)
            holding[i] = holding[i] + extra
            surplus = surplus - extra
    return np.array(holding)


def centred(key, extent, width, bound, split=(), held_as=jnp.bfloat16):
    factor_of = block_scale(key, extent, split, -0.22, 0.18) if split else 1.0
    entries = jax.random.normal(key, extent, jnp.float32) * width * factor_of
    return jnp.minimum(jnp.maximum(entries, -bound), bound).astype(held_as)


def setup_inputs(seed: int = 0, part: int = 0) -> dict:
    arg_keys = jax.random.split(jax.random.key(seed), 16)
    own_keys = jax.random.split(jax.random.fold_in(arg_keys[15], part), 16)
    queries = draw_queries(jax.random.fold_in(jax.random.fold_in(arg_keys[15], part), 71), part)
    key_values = draw_key_values(jax.random.fold_in(jax.random.fold_in(arg_keys[15], part), 71), part)
    query_gain = draw_query_gain(jax.random.fold_in(arg_keys[15], 71), part)
    key_gain = draw_key_gain(jax.random.fold_in(arg_keys[15], 71), part)
    out_weight = centred(arg_keys[4], (HQ * HEAD, D), (HQ * HEAD) ** -0.5, 0.1875, ((0, 4),))
    second_batch = centred(own_keys[5], (TOKENS_B, D), 1.0, 6.0, ((0, 16),))
    norm_gain = jnp.clip(1.0 + 0.18 * jax.random.normal(arg_keys[6], (D,), jnp.float32), 0.1, 1.9)
    routes_keys = jax.random.split(jax.random.fold_in(own_keys[7], 1), TOKENS_B // TOK_B)
    routes_turns = jax.random.permutation(jax.random.fold_in(own_keys[7], 3), TOKENS_B // TOK_B)
    routes = jax.vmap(lambda own, number: assign_block(jax.random.fold_in(own_keys[7], 2), own, number, TOK_B, EXPERTS, TOP_K, CAP, 2))(routes_keys, routes_turns).reshape((TOKENS_B, TOP_K))
    route_weights = jnp.clip(0.2 + 0.8 * jax.random.uniform(own_keys[8], (TOKENS_B, TOP_K), jnp.float32) ** block_scale(own_keys[8], (TOKENS_B, TOP_K), ((0, 16),), -0.2, 0.2), 0.2, 1.0)
    expert_gate = centred(arg_keys[9], (EXPERTS, D, EXPERT_HIDDEN), D ** -0.5, 0.125, ((0, 4), (2, 4)))
    expert_up = centred(arg_keys[10], (EXPERTS, D, EXPERT_HIDDEN), D ** -0.5, 0.125, ((0, 4), (2, 4)))
    expert_down = centred(arg_keys[11], (EXPERTS, EXPERT_HIDDEN, D), EXPERT_HIDDEN ** -0.5, 0.1875, ((0, 4), (1, 4)))
    shared_gate = centred(arg_keys[12], (D, SHARED), D ** -0.5, 0.125, ((1, 4),))
    shared_up = centred(arg_keys[13], (D, SHARED), D ** -0.5, 0.125, ((1, 4),))
    shared_down = centred(arg_keys[14], (SHARED, D), SHARED ** -0.5, 0.25, ((0, 4),))
    return dict(queries=queries, key_values=key_values, query_gain=query_gain, key_gain=key_gain, out_weight=out_weight, second_batch=second_batch, norm_gain=norm_gain, routes=routes, route_weights=route_weights, expert_gate=expert_gate, expert_up=expert_up, expert_down=expert_down, shared_gate=shared_gate, shared_up=shared_up, shared_down=shared_down)


rope_base = 10000.0
norm_eps = 1e-06

def head_norm(vectors, gain):
    return vectors * lax.rsqrt(lax.optimization_barrier(jnp.mean(vectors * vectors, axis=-1, keepdims=True)) + norm_eps) * gain

def turn_heads(vectors, positions):
    row_count, head_count, head_size = vectors.shape
    half_size = head_size // 2
    inverse = rope_base ** (-jnp.arange(0, half_size, 2, dtype=jnp.float32) / half_size)
    grid_row = (positions // GRID_W).astype(jnp.float32)
    grid_column = (positions % GRID_W).astype(jnp.float32)
    angles = jnp.concatenate([grid_row[:, None] * inverse, grid_column[:, None] * inverse], axis=-1)
    cosine = jnp.cos(angles)[:, None, :]
    sine = jnp.sin(angles)[:, None, :]
    paired = vectors.reshape(row_count, head_count, half_size, 2)
    first = paired[..., 0]
    second = paired[..., 1]
    turned = jnp.stack([first * cosine - second * sine, first * sine + second * cosine], axis=-1)
    return turned.reshape(vectors.shape)

def slot_ids(route_rows, expert_count, capacity):
    row_count, top_count = route_rows.shape
    flat_routes = route_rows.reshape(-1)
    onehot = (flat_routes[:, None] == jnp.arange(expert_count, dtype=jnp.int32)[None, :]).astype(jnp.int32)
    earlier = (jnp.cumsum(onehot, axis=0).astype(jnp.int32) - onehot).astype(jnp.int32)
    within = lax.optimization_barrier(jnp.sum(earlier * onehot, axis=1)).astype(jnp.int32)
    return (flat_routes * capacity + within).astype(jnp.int32).reshape(row_count, top_count)

def slot_table(slots, slot_count):
    row_count, top_count = slots.shape
    flat_slots = slots.reshape(-1)
    owner_row = jnp.arange(row_count * top_count, dtype=jnp.int32) // top_count
    matches = flat_slots[None, :] == jnp.arange(slot_count, dtype=jnp.int32)[:, None]
    occupied = jnp.any(matches, axis=1)
    source_row = lax.optimization_barrier(jnp.sum(jnp.where(matches, owner_row[None, :], 0), axis=1)).astype(jnp.int32)
    return jnp.where(occupied, source_row, row_count).astype(jnp.int32)

def block_sum(hidden, down_weights, block_width):
    summed = jnp.zeros((hidden.shape[0], down_weights.shape[1]), jnp.float32)
    for block_index in range(hidden.shape[1] // block_width):
        lower = block_index * block_width
        partial_value = jnp.dot(hidden[:, lower:lower + block_width], down_weights[lower:lower + block_width], preferred_element_type=jnp.float32).astype(jnp.bfloat16)
        summed = summed + lax.optimization_barrier(partial_value).astype(jnp.float32)
    return summed

def swiglu_hidden(token_rows, gate_weights, up_weights):
    gate_part = jnp.dot(token_rows, gate_weights, preferred_element_type=jnp.float32)
    up_part = jnp.dot(token_rows, up_weights, preferred_element_type=jnp.float32)
    return (jax.nn.silu(gate_part) * up_part).astype(jnp.bfloat16)

def expert_apply(operands):
    slot_rows, gate_weights, up_weights, down_weights = operands
    hidden = swiglu_hidden(slot_rows, gate_weights, up_weights)
    return block_sum(hidden, down_weights, FE_DEV).astype(jnp.bfloat16)

def reference(queries, key_values, query_gain, key_gain, out_weight, second_batch, norm_gain, routes, route_weights, expert_gate, expert_up, expert_down, shared_gate, shared_up, shared_down):
    total_rows = queries.shape[0]
    positions = jnp.arange(total_rows, dtype=jnp.int32)
    query_turned = turn_heads(head_norm(queries.reshape(total_rows, HQ, HEAD).astype(jnp.float32), query_gain), positions).astype(jnp.bfloat16)
    query_turned = lax.optimization_barrier(query_turned)
    pairs = key_values.reshape(total_rows, KV_HEADS, 2 * HEAD)
    key_turned = turn_heads(head_norm(pairs[:, :, :HEAD].astype(jnp.float32), key_gain), positions).astype(jnp.bfloat16)
    key_float = lax.optimization_barrier(key_turned).astype(jnp.float32)
    value_float = pairs[:, :, HEAD:].astype(jnp.float32)
    scale = HEAD ** (-0.5)

    def query_block(block_queries):
        summed = jnp.zeros((block_queries.shape[0], D), jnp.float32)
        for head_group in range(KV_HEADS):
            group_queries = block_queries[:, head_group * HQ_DEV:(head_group + 1) * HQ_DEV].astype(jnp.float32)
            scores = jnp.einsum('qhd,kd->hqk', group_queries, key_float[:, head_group]) * scale
            top = lax.optimization_barrier(jnp.max(scores, axis=-1, keepdims=True))
            exps = jnp.exp(scores - top)
            totals = lax.optimization_barrier(jnp.sum(exps, axis=-1))
            weights = lax.optimization_barrier(exps.astype(jnp.bfloat16)).astype(jnp.float32)
            numerators = jnp.einsum('hqk,kd->qhd', weights, value_float[:, head_group])
            head_out = (numerators / totals.T[:, :, None]).astype(jnp.bfloat16).reshape(-1, HQ_DEV * HEAD)
            lower = head_group * HQ_DEV * HEAD
            partial_value = jnp.dot(head_out, out_weight[lower:lower + HQ_DEV * HEAD], preferred_element_type=jnp.float32).astype(jnp.bfloat16)
            summed = summed + lax.optimization_barrier(partial_value).astype(jnp.float32)
        return summed.astype(jnp.bfloat16)
    mixer_out = lax.map(query_block, query_turned.reshape(N_EP, TOK_A, HQ, HEAD)).reshape(total_rows, D)
    token_float = second_batch.astype(jnp.float32)
    normed = (token_float * lax.rsqrt(lax.optimization_barrier(jnp.mean(token_float * token_float, axis=-1, keepdims=True)) + norm_eps) * norm_gain).astype(jnp.bfloat16)
    block_count = normed.shape[0] // TOK_B
    slot_count = EXPERTS * CAP
    slots = jax.vmap(lambda route_rows: slot_ids(route_rows, EXPERTS, CAP))(routes.reshape(block_count, TOK_B, TOP_K))
    tables = jax.vmap(lambda slot_block: slot_table(slot_block, slot_count))(slots)
    inputs = jax.vmap(lambda token_rows, table_rows: jnp.take(token_rows, table_rows, axis=0, mode='fill', fill_value=0))(normed.reshape(block_count, TOK_B, D), tables)
    per_expert = inputs.reshape(block_count, EXPERTS, CAP, D).transpose(1, 0, 2, 3).reshape(EXPERTS, block_count * CAP, D)
    outputs = lax.map(expert_apply, (per_expert, expert_gate, expert_up, expert_down))
    by_block = outputs.reshape(EXPERTS, block_count, CAP, D).transpose(1, 0, 2, 3).reshape(block_count, slot_count, D)
    chosen = jax.vmap(lambda block_out, slot_block: jnp.take(block_out, slot_block.reshape(-1), axis=0))(by_block, slots).reshape(-1, TOP_K, D)
    routed = lax.optimization_barrier(jnp.sum(route_weights[:, :, None] * chosen.astype(jnp.float32), axis=1))
    shared_hidden = swiglu_hidden(normed, shared_gate, shared_up)
    shared_sum = block_sum(shared_hidden, shared_down, SH_DEV)
    channel_out = (shared_sum + routed).astype(jnp.bfloat16)
    return (mixer_out, channel_out)
```

```python
import functools

import jax
import jax.numpy as jnp
from jax import lax
from jax.experimental import pallas as pl
from jax.experimental.pallas import tpu as pltpu
from jax.sharding import PartitionSpec as P

GRID_W = 64


rope_base = 10000.0
norm_eps = 1e-06


def head_norm(vectors, gain):
    return (
        vectors * lax.rsqrt(jnp.mean(vectors * vectors, axis=-1, keepdims=True) + norm_eps) * gain
    )


def turn_heads(vectors, positions):
    row_count, head_count, head_size = vectors.shape
    half_size = head_size // 2
    inverse = rope_base ** (-jnp.arange(0, half_size, 2, dtype=jnp.float32) / half_size)
    grid_row = (positions // GRID_W).astype(jnp.float32)
    grid_column = (positions % GRID_W).astype(jnp.float32)
    angles = jnp.concatenate([grid_row[:, None] * inverse, grid_column[:, None] * inverse], axis=-1)
    cosine = jnp.cos(angles)[:, None, :]
    sine = jnp.sin(angles)[:, None, :]
    paired = vectors.reshape(row_count, head_count, half_size, 2)
    first = paired[..., 0]
    second = paired[..., 1]
    turned = jnp.stack([first * cosine - second * sine, first * sine + second * cosine], axis=-1)
    return turned.reshape(vectors.shape)


def slot_ids(route_rows, expert_count, capacity):
    row_count, top_count = route_rows.shape
    flat_routes = route_rows.reshape(-1)
    pair_count = row_count * top_count
    onehot = flat_routes[:, None] == jnp.arange(expert_count, dtype=jnp.int32)[None, :]
    order = jnp.arange(pair_count, dtype=jnp.int32)
    before = (order[None, :] < order[:, None]).astype(jnp.bfloat16)
    earlier = jnp.dot(before, onehot.astype(jnp.bfloat16), preferred_element_type=jnp.float32)
    within = jnp.sum(jnp.where(onehot, earlier, 0.0), axis=1).astype(jnp.int32)
    return (flat_routes * capacity + within).reshape(row_count, top_count)


MESH = pl.DeviceIdType.MESH


def greet(ep_count, tp_count, e, t):
    barrier = pltpu.get_barrier_semaphore()
    peers = 0
    for d in range(1, ep_count):
        pl.semaphore_signal(
            barrier, inc=1, device_id={"ep": lax.rem(e + d, ep_count)}, device_id_type=MESH
        )
        peers += 1
    pair = t // 2
    core = lax.rem(t, 2)
    for k in range(1, tp_count // 2):
        pl.semaphore_signal(
            barrier,
            inc=1,
            device_id={"tp": lax.rem(pair + k, tp_count // 2) * 2 + core},
            device_id_type=MESH,
        )
        peers += 1
    pl.semaphore_signal(
        barrier, inc=1, device_id={"tp": pair * 2 + 1 - core}, device_id_type=MESH
    )
    peers += 1
    pl.semaphore_wait(barrier, peers)


def remote(src, dst, send, recv, device):
    return pltpu.make_async_remote_copy(
        src_ref=src,
        dst_ref=dst,
        send_sem=send,
        recv_sem=recv,
        device_id=device,
        device_id_type=MESH,
    )


def dispatch_kernel(
    ep_count,
    tp_count,
    blocks,
    normed,
    kv,
    arrived,
    normed_all,
    kv_all,
    local_sem,
    kv_send,
    kv_recv,
    z_send,
    z_recv,
    x_send,
    x_recv,
    d_send,
    d_recv,
):
    e = lax.axis_index("ep")
    t = lax.axis_index("tp")
    half = tp_count // 2
    pair = t // 2
    core = lax.rem(t, 2)
    sibling = {"tp": pair * 2 + 1 - core}
    greet(ep_count, tp_count, e, t)

    sends = []
    for d in range(1, ep_count):
        there = lax.rem(e + d, ep_count)
        copy = remote(kv, kv_all.at[e], kv_send.at[d], kv_recv.at[e], {"ep": there})
        copy.start()
        sends.append(copy)
    for d in range(1, ep_count):
        there = lax.rem(e + d, ep_count)
        copy = remote(
            blocks.at[there], arrived.at[:, t, e], z_send.at[d], z_recv.at[e], {"ep": there}
        )
        copy.start()
        sends.append(copy)

    def place(item, row):
        if item is None:
            return normed_all.at[row]
        return arrived.at[:, row, item]

    def spread(src, item, number):
        for k in range(1, half):
            other = lax.rem(pair + k, half)
            copy = remote(
                src,
                place(item, t),
                x_send.at[k, number],
                x_recv.at[pair, number],
                {"tp": other * 2 + core},
            )
            copy.start()
            sends.append(copy)
        copy = remote(
            src, place(item, t), d_send.at[0, number], d_recv.at[pair, number], sibling
        )
        copy.start()
        sends.append(copy)

    def pass_on(item, number):
        for k in range(1, half):
            other = lax.rem(pair + k, half)
            row = other * 2 + core
            spot = place(item, row)
            remote(spot, spot, x_send.at[k, number], x_recv.at[other, number], sibling).wait_recv()
            copy = remote(spot, spot, d_send.at[k, number], d_recv.at[other, number], sibling)
            copy.start()
            sends.append(copy)

    spread(blocks.at[e], e, 0)
    spread(normed, None, ep_count)
    own = [
        pltpu.make_async_copy(blocks.at[e], arrived.at[:, t, e], local_sem.at[0]),
        pltpu.make_async_copy(normed, normed_all.at[t], local_sem.at[1]),
        pltpu.make_async_copy(kv, kv_all.at[e], local_sem.at[2]),
    ]
    for copy in own:
        copy.start()

    pass_on(e, 0)
    pass_on(None, ep_count)
    for d in range(1, ep_count):
        source = lax.rem(e - d + ep_count, ep_count)
        spot = arrived.at[:, t, source]
        remote(spot, spot, z_send.at[d], z_recv.at[source], sibling).wait_recv()
        spread(spot, source, d)
        if d > 1:
            pass_on(lax.rem(e - d + 1 + ep_count, ep_count), d - 1)
    if ep_count > 1:
        pass_on(lax.rem(e + 1, ep_count), ep_count - 1)

    for d in range(1, ep_count):
        source = lax.rem(e - d + ep_count, ep_count)
        spot = kv_all.at[source]
        remote(spot, spot, kv_send.at[d], kv_recv.at[source], sibling).wait_recv()
    for number in range(ep_count + 1):
        item = None if number == ep_count else lax.rem(e - number + ep_count, ep_count)
        for other in range(half):
            spot = place(item, other * 2 + 1 - core)
            remote(spot, spot, d_send.at[0, number], d_recv.at[other, number], sibling).wait_recv()
    for copy in own:
        copy.wait()
    for copy in sends:
        copy.wait_send()


def dispatch(ep_count, tp_count, blocks, normed, kv):
    locals_here, capacity, width = blocks.shape[1:]
    vmem = pl.BlockSpec(memory_space=pltpu.VMEM)
    half = tp_count // 2
    dma = pltpu.SemaphoreType.DMA
    return pl.pallas_call(
        functools.partial(dispatch_kernel, ep_count, tp_count),
        out_shape=(
            jax.ShapeDtypeStruct(
                (locals_here, tp_count, ep_count, capacity, width), jnp.bfloat16
            ),
            jax.ShapeDtypeStruct((tp_count,) + normed.shape, jnp.bfloat16),
            jax.ShapeDtypeStruct((ep_count,) + kv.shape, jnp.bfloat16),
        ),
        in_specs=[vmem] * 3,
        out_specs=(vmem,) * 3,
        scratch_shapes=[
            dma((3,)),
            dma((ep_count,)),
            dma((ep_count,)),
            dma((ep_count,)),
            dma((ep_count,)),
            dma((half, ep_count + 1)),
            dma((half, ep_count + 1)),
            dma((half, ep_count + 1)),
            dma((half, ep_count + 1)),
        ],
        compiler_params=pltpu.CompilerParams(collective_id=0, has_side_effects=True),
    )(blocks, normed, kv)


def collect_kernel(
    ep_count,
    tp_count,
    routed,
    shared,
    mixed,
    returned,
    shared_sum,
    mixed_sum,
    routed_pair,
    routed_out,
    routed_in,
    routed_done,
    shared_pair,
    shared_out,
    shared_in,
    mixed_pair,
    mixed_out,
    mixed_in,
    d_send,
    d_recv,
    x_send,
    x_recv,
    z_send,
    z_recv,
):
    e = lax.axis_index("ep")
    t = lax.axis_index("tp")
    half = tp_count // 2
    pair = t // 2
    core = lax.rem(t, 2)
    sibling = {"tp": pair * 2 + 1 - core}
    greet(ep_count, tp_count, e, t)

    def item(number):
        if number < ep_count:
            place = lax.rem(e + number + 1, ep_count)
            return (
                lambda row: routed.at[:, row, place],
                lambda k: routed_pair.at[number, k],
                lambda k: routed_out.at[number, k],
                lambda k: routed_in.at[number, k],
            )
        if number == ep_count:
            return (
                lambda row: shared.at[row],
                lambda k: shared_pair.at[k],
                lambda k: shared_out.at[k],
                lambda k: shared_in.at[k],
            )
        return (
            lambda row: mixed.at[row],
            lambda k: mixed_pair.at[k],
            lambda k: mixed_out.at[k],
            lambda k: mixed_in.at[k],
        )

    count = ep_count + 2
    sends = []
    for number in range(count):
        part, paired, out, into = item(number)
        for k in list(range(1, half)) + [0]:
            other = lax.rem(pair + k, half)
            copy = remote(
                part(other * 2 + 1 - core),
                paired(k),
                d_send.at[number, k],
                d_recv.at[number, k],
                sibling,
            )
            copy.start()
            sends.append(copy)

    def both(number, k):
        part, paired, out, into = item(number)
        spot = paired(k)
        remote(spot, spot, d_send.at[number, k], d_recv.at[number, k], sibling).wait_recv()
        mine = part(lax.rem(pair + k, half) * 2 + core)
        return mine[...].astype(jnp.float32) + spot[...].astype(jnp.float32)

    for number in range(count):
        part, paired, out, into = item(number)
        for k in range(1, half):
            other = lax.rem(pair + k, half)
            out(k)[...] = both(number, k).astype(jnp.bfloat16)
            copy = remote(
                out(k),
                into(k),
                x_send.at[number, k],
                x_recv.at[number, k],
                {"tp": other * 2 + core},
            )
            copy.start()
            sends.append(copy)
    for number in range(count):
        part, paired, out, into = item(number)
        total = both(number, 0)
        for k in range(1, half):
            spot = into(k)
            remote(spot, spot, x_send.at[number, k], x_recv.at[number, k], sibling).wait_recv()
            total = total + spot[...].astype(jnp.float32)
        if number < ep_count - 1:
            place = lax.rem(e + number + 1, ep_count)
            routed_done[number] = total.astype(jnp.bfloat16)
            copy = remote(
                routed_done.at[number],
                returned.at[e],
                z_send.at[number],
                z_recv.at[e],
                {"ep": place},
            )
            copy.start()
            sends.append(copy)
        elif number == ep_count - 1:
            returned[e] = total.astype(jnp.bfloat16)
        elif number == ep_count:
            shared_sum[...] = total
        else:
            mixed_sum[...] = total.astype(jnp.bfloat16)
    for d in range(1, ep_count):
        source = lax.rem(e - d + ep_count, ep_count)
        spot = returned.at[source]
        remote(spot, spot, z_send.at[0], z_recv.at[source], sibling).wait_recv()
    for copy in sends:
        copy.wait_send()


def collect(ep_count, tp_count, routed, shared, mixed):
    locals_here, capacity, width = routed.shape[0], routed.shape[3], routed.shape[4]
    vmem = pl.BlockSpec(memory_space=pltpu.VMEM)
    half = tp_count // 2
    dma = pltpu.SemaphoreType.DMA
    block = (locals_here, capacity, width)
    count = ep_count + 2
    return pl.pallas_call(
        functools.partial(collect_kernel, ep_count, tp_count),
        out_shape=(
            jax.ShapeDtypeStruct((ep_count,) + block, jnp.bfloat16),
            jax.ShapeDtypeStruct(shared.shape[1:], jnp.float32),
            jax.ShapeDtypeStruct(mixed.shape[1:], jnp.bfloat16),
        ),
        in_specs=[vmem] * 3,
        out_specs=(vmem,) * 3,
        scratch_shapes=[
            pltpu.VMEM((ep_count, half) + block, jnp.bfloat16),
            pltpu.VMEM((ep_count, half) + block, jnp.bfloat16),
            pltpu.VMEM((ep_count, half) + block, jnp.bfloat16),
            pltpu.VMEM((ep_count,) + block, jnp.bfloat16),
            pltpu.VMEM((half,) + shared.shape[1:], jnp.bfloat16),
            pltpu.VMEM((half,) + shared.shape[1:], jnp.bfloat16),
            pltpu.VMEM((half,) + shared.shape[1:], jnp.bfloat16),
            pltpu.VMEM((half,) + mixed.shape[1:], jnp.bfloat16),
            pltpu.VMEM((half,) + mixed.shape[1:], jnp.bfloat16),
            pltpu.VMEM((half,) + mixed.shape[1:], jnp.bfloat16),
            dma((count, half)),
            dma((count, half)),
            dma((count, half)),
            dma((count, half)),
            dma((ep_count,)),
            dma((ep_count,)),
        ],
        compiler_params=pltpu.CompilerParams(
            collective_id=1, has_side_effects=True, vmem_limit_bytes=67043328
        ),
    )(routed, shared, mixed)


def pick_block(row_count):
    for candidate in range(min(row_count, 1024), 0, -1):
        if row_count % candidate == 0:
            return candidate
    return row_count


def attend_keys(query_turned, scale, running, pieces):
    head_size = query_turned.shape[-1]
    key_block = pick_block(pieces.shape[0])
    blocks = pieces.reshape(pieces.shape[0] // key_block, key_block, 2 * head_size)

    def one_block(carried, block_rows):
        top_now, total_now, acc_now = carried
        scores = (
            jnp.einsum(
                "qhd,kd->hqk",
                query_turned,
                block_rows[:, :head_size],
                preferred_element_type=jnp.float32,
            )
            * scale
        )
        top_new = jnp.maximum(top_now, jnp.max(scores, axis=-1))
        shrink = jnp.exp(top_now - top_new)
        exps = jnp.exp(scores - top_new[..., None])
        total_new = total_now * shrink + jnp.sum(exps, axis=-1)
        acc_new = acc_now * shrink[..., None] + jnp.einsum(
            "hqk,kd->hqd",
            exps.astype(jnp.bfloat16),
            block_rows[:, head_size:],
            preferred_element_type=jnp.float32,
        )
        return ((top_new, total_new, acc_new), None)

    result, ignored = lax.scan(one_block, running, blocks)
    return result


def shared_hidden_of(token_rows, gate_weights, up_weights):
    gate_part = jnp.dot(token_rows, gate_weights, preferred_element_type=jnp.float32)
    up_part = jnp.dot(token_rows, up_weights, preferred_element_type=jnp.float32)
    return (jax.nn.silu(gate_part) * up_part).astype(jnp.bfloat16)


def body(
    queries,
    key_values,
    query_gain,
    key_gain,
    out_weight,
    second_batch,
    norm_gain,
    routes,
    route_weights,
    expert_gate,
    expert_up,
    expert_down,
    shared_gate,
    shared_up,
    shared_down,
):
    query_rows = queries.shape[0]
    head_size = query_gain.shape[0]
    heads_here = queries.shape[1] // head_size
    ep_count = lax.axis_size("ep")
    tp_count = lax.axis_size("tp")
    positions = lax.axis_index("ep") * query_rows + jnp.arange(query_rows, dtype=jnp.int32)
    query_turned = turn_heads(
        head_norm(
            queries.reshape(query_rows, heads_here, head_size).astype(jnp.float32), query_gain
        ),
        positions,
    ).astype(jnp.bfloat16)
    key_turned = turn_heads(
        head_norm(key_values[:, None, :head_size].astype(jnp.float32), key_gain), positions
    ).astype(jnp.bfloat16)
    keys_and_values = jnp.concatenate([key_turned[:, 0, :], key_values[:, head_size:]], axis=1)
    tok_count = second_batch.shape[0]
    model_width = second_batch.shape[1]
    top_count = routes.shape[1]
    local_experts = expert_gate.shape[0]
    expert_count = local_experts * ep_count
    capacity = 3 * tok_count * top_count // (2 * expert_count)
    slot_count = expert_count * capacity
    token_float = second_batch.astype(jnp.float32)
    normed = (
        token_float
        * lax.rsqrt(jnp.mean(token_float * token_float, axis=-1, keepdims=True) + norm_eps)
        * norm_gain
    ).astype(jnp.bfloat16)
    own_slots = slot_ids(routes, expert_count, capacity)
    slot_numbers = jnp.arange(slot_count, dtype=jnp.int32)
    picks = [
        (own_slots[:, j][:, None] == slot_numbers[None, :]).astype(jnp.bfloat16)
        for j in range(top_count)
    ]
    outgoing = lax.dot_general(
        sum(picks), normed, (((0,), (0,)), ((), ())), preferred_element_type=jnp.float32
    ).astype(jnp.bfloat16)
    arrived, normed_all, kv_all = dispatch(
        ep_count,
        tp_count,
        outgoing.reshape(ep_count, local_experts, capacity, model_width),
        normed,
        keys_and_values,
    )
    start_state = (
        jnp.full((heads_here, query_rows), -1e30, jnp.float32),
        jnp.zeros((heads_here, query_rows), jnp.float32),
        jnp.zeros((heads_here, query_rows, head_size), jnp.float32),
    )
    top_all, total_all, acc_all = attend_keys(
        query_turned,
        head_size ** (-0.5),
        start_state,
        kv_all.reshape(ep_count * query_rows, 2 * head_size),
    )
    head_out = (
        (acc_all / total_all[..., None])
        .transpose(1, 0, 2)
        .reshape(query_rows, heads_here * head_size)
        .astype(jnp.bfloat16)
    )
    head_partial = jnp.dot(head_out, out_weight, preferred_element_type=jnp.float32)
    shared_hidden = shared_hidden_of(
        normed_all.reshape(tp_count * tok_count, model_width), shared_gate, shared_up
    )
    shared_part = jnp.dot(shared_hidden, shared_down, preferred_element_type=jnp.float32)
    slot_rows = arrived.reshape(local_experts, tp_count * ep_count * capacity, model_width)
    gate_part = jnp.einsum(
        "jmd,jdf->jmf", slot_rows, expert_gate, preferred_element_type=jnp.float32
    )
    up_part = jnp.einsum("jmd,jdf->jmf", slot_rows, expert_up, preferred_element_type=jnp.float32)
    hidden = (jax.nn.silu(gate_part) * up_part).astype(jnp.bfloat16)
    routed_part = jnp.einsum(
        "jmf,jfd->jmd", hidden, expert_down, preferred_element_type=jnp.float32
    )
    returned, shared_sum, mixer_out = collect(
        ep_count,
        tp_count,
        routed_part.astype(jnp.bfloat16).reshape(arrived.shape),
        shared_part.astype(jnp.bfloat16).reshape(normed_all.shape),
        head_partial.astype(jnp.bfloat16).reshape(tp_count, query_rows // tp_count, model_width),
    )
    returned = returned.reshape(slot_count, model_width)
    combined = shared_sum
    for j in range(top_count):
        combined = combined + route_weights[:, j : j + 1] * jnp.dot(
            picks[j], returned, preferred_element_type=jnp.float32
        )
    return (mixer_out, combined.astype(jnp.bfloat16))


def solution(mesh):
    placed = (
        P(("grp", "ep"), "tp"),
        P(("grp", "ep"), "tp"),
        P(),
        P(),
        P("tp", None),
        P(("grp", "ep", "tp"), None),
        P(),
        P(("grp", "ep", "tp"), None),
        P(("grp", "ep", "tp"), None),
        P("ep", None, "tp"),
        P("ep", None, "tp"),
        P("ep", "tp", None),
        P(None, "tp"),
        P(None, "tp"),
        P("tp", None),
    )
    return jax.shard_map(
        body,
        mesh=mesh,
        in_specs=placed,
        out_specs=(P(("grp", "ep", "tp"), None), P(("grp", "ep", "tp"), None)),
        check_vma=False,
    )
```

```python
import functools

import jax
import jax.numpy as jnp
from jax import lax
from jax.experimental import pallas as pl
from jax.experimental.pallas import tpu as pltpu
from jax.sharding import PartitionSpec as P

GRID_W = 64


rope_base = 10000.0
norm_eps = 1e-06


def head_norm(vectors, gain):
    return (
        vectors * lax.rsqrt(jnp.mean(vectors * vectors, axis=-1, keepdims=True) + norm_eps) * gain
    )


def turn_heads(vectors, positions):
    row_count, head_count, head_size = vectors.shape
    half_size = head_size // 2
    inverse = rope_base ** (-jnp.arange(0, half_size, 2, dtype=jnp.float32) / half_size)
    grid_row = (positions // GRID_W).astype(jnp.float32)
    grid_column = (positions % GRID_W).astype(jnp.float32)
    angles = jnp.concatenate([grid_row[:, None] * inverse, grid_column[:, None] * inverse], axis=-1)
    cosine = jnp.cos(angles)[:, None, :]
    sine = jnp.sin(angles)[:, None, :]
    paired = vectors.reshape(row_count, head_count, half_size, 2)
    first = paired[..., 0]
    second = paired[..., 1]
    turned = jnp.stack([first * cosine - second * sine, first * sine + second * cosine], axis=-1)
    return turned.reshape(vectors.shape)


def slot_ids(route_rows, expert_count, capacity):
    row_count, top_count = route_rows.shape
    flat_routes = route_rows.reshape(-1)
    pair_count = row_count * top_count
    onehot = flat_routes[:, None] == jnp.arange(expert_count, dtype=jnp.int32)[None, :]
    order = jnp.arange(pair_count, dtype=jnp.int32)
    before = (order[None, :] < order[:, None]).astype(jnp.bfloat16)
    earlier = jnp.dot(before, onehot.astype(jnp.bfloat16), preferred_element_type=jnp.float32)
    within = jnp.sum(jnp.where(onehot, earlier, 0.0), axis=1).astype(jnp.int32)
    return (flat_routes * capacity + within).reshape(row_count, top_count)


MESH = pl.DeviceIdType.MESH


def greet(ep_count, tp_count, e, t):
    barrier = pltpu.get_barrier_semaphore()
    peers = 0
    for d in range(1, ep_count):
        pl.semaphore_signal(
            barrier, inc=1, device_id={"ep": lax.rem(e + d, ep_count)}, device_id_type=MESH
        )
        peers += 1
    pair = t // 2
    core = lax.rem(t, 2)
    for k in range(1, tp_count // 2):
        pl.semaphore_signal(
            barrier,
            inc=1,
            device_id={"tp": lax.rem(pair + k, tp_count // 2) * 2 + core},
            device_id_type=MESH,
        )
        peers += 1
    pl.semaphore_signal(
        barrier, inc=1, device_id={"tp": pair * 2 + 1 - core}, device_id_type=MESH
    )
    peers += 1
    pl.semaphore_wait(barrier, peers)


def remote(src, dst, send, recv, device):
    return pltpu.make_async_remote_copy(
        src_ref=src,
        dst_ref=dst,
        send_sem=send,
        recv_sem=recv,
        device_id=device,
        device_id_type=MESH,
    )


def whole_kernel(
    ep_count,
    tp_count,
    blocks,
    normed,
    kv,
    query,
    out_weight_hbm,
    gate_hbm,
    up_hbm,
    down_hbm,
    shared_gate_hbm,
    shared_up_hbm,
    shared_down_hbm,
    returned,
    shared_sum,
    mixed_sum,
    arrived,
    normed_all,
    kv_all,
    out_weight,
    gate,
    up,
    down,
    shared_gate,
    shared_up,
    shared_down,
    heads_scr,
    routed,
    shared,
    mixed,
    routed_pair,
    routed_out,
    routed_in,
    routed_done,
    shared_pair,
    shared_out,
    shared_in,
    mixed_pair,
    mixed_out,
    mixed_in,
    local_sem,
    kv_send,
    kv_recv,
    z_send,
    z_recv,
    x_send,
    x_recv,
    d_send,
    d_recv,
    back_d_send,
    back_d_recv,
    back_x_send,
    back_x_recv,
    back_z_send,
    back_z_recv,
):
    e = lax.axis_index("ep")
    t = lax.axis_index("tp")
    half = tp_count // 2
    pair = t // 2
    core = lax.rem(t, 2)
    sibling = {"tp": pair * 2 + 1 - core}
    f32 = jnp.float32
    bf16 = jnp.bfloat16
    loads = [
        pltpu.make_async_copy(source, target, local_sem.at[3 + n])
        for n, (source, target) in enumerate(
            (
                (out_weight_hbm, out_weight),
                (gate_hbm, gate),
                (up_hbm, up),
                (down_hbm, down),
                (shared_gate_hbm, shared_gate),
                (shared_up_hbm, shared_up),
                (shared_down_hbm, shared_down),
            )
        )
    ]
    for copy in loads:
        copy.start()
    greet(ep_count, tp_count, e, t)

    sends = []

    def send(src, dst, send_sem, recv_sem, device):
        copy = remote(src, dst, send_sem, recv_sem, device)
        copy.start()
        sends.append(copy)

    def landed(spot, recv_sem):
        remote(spot, spot, kv_send.at[0], recv_sem, sibling).wait_recv()

    def source_of(d):
        return lax.rem(e - d + ep_count, ep_count)

    def place(d, row):
        if d == ep_count:
            return normed_all.at[row]
        return arrived.at[:, row, source_of(d)]

    for d in range(1, ep_count):
        there = lax.rem(e + d, ep_count)
        send(kv, kv_all.at[e], kv_send.at[d], kv_recv.at[e], {"ep": there})
    for d in range(1, ep_count):
        there = lax.rem(e + d, ep_count)
        send(blocks.at[there], arrived.at[:, t, e], z_send.at[d], z_recv.at[e], {"ep": there})

    def spread(src, d):
        for k in range(1, half):
            other = lax.rem(pair + k, half)
            send(
                src,
                place(d, t),
                x_send.at[k, d],
                x_recv.at[pair, d],
                {"tp": other * 2 + core},
            )
        send(src, place(d, t), d_send.at[0, d], d_recv.at[pair, d], sibling)

    def pass_on(d):
        for k in range(1, half):
            other = lax.rem(pair + k, half)
            spot = place(d, other * 2 + core)
            landed(spot, x_recv.at[other, d])
            send(spot, spot, d_send.at[k, d], d_recv.at[other, d], sibling)

    def come(d):
        spot = arrived.at[:, t, source_of(d)]
        landed(spot, z_recv.at[source_of(d)])
        spread(spot, d)

    def all_here(d):
        for other in range(half):
            landed(place(d, other * 2 + 1 - core), d_recv.at[other, d])

    spread(blocks.at[e], 0)
    spread(normed, ep_count)
    own = [
        pltpu.make_async_copy(blocks.at[e], arrived.at[:, t, e], local_sem.at[0]),
        pltpu.make_async_copy(normed, normed_all.at[t], local_sem.at[1]),
        pltpu.make_async_copy(kv, kv_all.at[e], local_sem.at[2]),
    ]
    for copy in own:
        copy.start()

    query_rows, wide = query.shape[1], query.shape[2]
    model_width = normed.shape[1]
    tile = min(512, model_width)

    def attend(h):
        def step(b, carried):
            top_now, total_now, acc_now = carried
            block = kv_all[b]
            scores = lax.dot_general(
                query[h], block, (((1,), (1,)), ((), ())), preferred_element_type=f32
            )
            top_new = jnp.maximum(top_now, jnp.max(scores, axis=-1, keepdims=True))
            shrink = jnp.exp(top_now - top_new)
            exps = jnp.exp(scores - top_new)
            total_new = total_now * shrink + jnp.sum(exps, axis=-1, keepdims=True)
            acc_new = acc_now * shrink + jnp.dot(
                exps.astype(bf16), block, preferred_element_type=f32
            )
            return (top_new, total_new, acc_new)

        start = (
            jnp.full((query_rows, 1), -1e30, f32),
            jnp.zeros((query_rows, 1), f32),
            jnp.zeros((query_rows, wide), f32),
        )
        top, total, acc = lax.fori_loop(0, ep_count, step, start)
        return acc / total

    def attend_two(n):
        low = pltpu.roll(attend(2 * n), wide // 2, 1)
        high = attend(2 * n + 1)
        lane = lax.broadcasted_iota(jnp.int32, low.shape, 1)
        heads_scr[:, n * wide : (n + 1) * wide] = jnp.where(lane < wide // 2, low, high).astype(
            bf16
        )

    def project():
        def step(n, ignored):
            columns = pl.ds(pl.multiple_of(n * tile, tile), tile)
            part = jnp.dot(heads_scr[...], out_weight[:, columns], preferred_element_type=f32)
            mixed[:, :, columns] = part.astype(bf16).reshape(
                tp_count, query_rows // tp_count, tile
            )
            return ignored

        lax.fori_loop(0, model_width // tile, step, 0)

    def share():
        def step(row, ignored):
            rows = normed_all[row]
            gate_part = jnp.dot(rows, shared_gate[...], preferred_element_type=f32)
            up_part = jnp.dot(rows, shared_up[...], preferred_element_type=f32)
            hidden = (gate_part / (1.0 + jnp.exp(-gate_part)) * up_part).astype(bf16)
            shared[row] = jnp.dot(hidden, shared_down[...], preferred_element_type=f32).astype(
                bf16
            )
            return ignored

        lax.fori_loop(0, tp_count, step, 0)

    local_count, capacity = arrived.shape[0], arrived.shape[3]

    def experts(d):
        source = source_of(d)

        def step(n, ignored):
            rows = arrived[n, :, source]
            if capacity % 16:
                rows = rows.astype(f32)
            rows = rows.reshape(tp_count * capacity, model_width).astype(bf16)
            gate_part = jnp.dot(rows, gate[n], preferred_element_type=f32)
            up_part = jnp.dot(rows, up[n], preferred_element_type=f32)
            hidden = (gate_part / (1.0 + jnp.exp(-gate_part)) * up_part).astype(bf16)

            def columns_step(m, inner):
                columns = pl.ds(pl.multiple_of(m * tile, tile), tile)
                part = jnp.dot(hidden, down[n, :, columns], preferred_element_type=f32)
                if capacity % 16:
                    part = part.reshape(tp_count, capacity, tile).astype(bf16)
                else:
                    part = part.astype(bf16).reshape(tp_count, capacity, tile)
                routed[n, :, source, :, columns] = part
                return inner

            lax.fori_loop(0, model_width // tile, columns_step, 0)
            return ignored

        lax.fori_loop(0, local_count, step, 0)

    def item(d):
        if d < ep_count:
            source = source_of(d)
            return (
                lambda row: routed.at[:, row, source],
                lambda k: routed_pair.at[d, k],
                lambda k: routed_out.at[d, k - 1],
                lambda k: routed_in.at[d, k - 1],
            )
        if d == ep_count:
            return (
                lambda row: shared.at[row],
                lambda k: shared_pair.at[k],
                lambda k: shared_out.at[k - 1],
                lambda k: shared_in.at[k - 1],
            )
        return (
            lambda row: mixed.at[row],
            lambda k: mixed_pair.at[k],
            lambda k: mixed_out.at[k - 1],
            lambda k: mixed_in.at[k - 1],
        )

    def to_sibling(d):
        part, paired, out, into = item(d)
        for k in list(range(1, half)) + [0]:
            other = lax.rem(pair + k, half)
            send(
                part(other * 2 + 1 - core),
                paired(k),
                back_d_send.at[d, k],
                back_d_recv.at[d, k],
                sibling,
            )

    def both(d, k):
        part, paired, out, into = item(d)
        spot = paired(k)
        landed(spot, back_d_recv.at[d, k])
        mine = part(lax.rem(pair + k, half) * 2 + core)
        return mine[...].astype(f32) + spot[...].astype(f32)

    crossed = set()

    def across(d):
        if d in crossed:
            return
        crossed.add(d)
        part, paired, out, into = item(d)
        for k in range(1, half):
            other = lax.rem(pair + k, half)
            out(k)[...] = both(d, k).astype(bf16)
            send(
                out(k),
                into(k),
                back_x_send.at[d, k],
                back_x_recv.at[d, k],
                {"tp": other * 2 + core},
            )

    finished = set()

    def finish(d):
        if d in finished:
            return
        finished.add(d)
        part, paired, out, into = item(d)
        total = both(d, 0)
        for k in range(1, half):
            spot = into(k)
            landed(spot, back_x_recv.at[d, k])
            total = total + spot[...].astype(f32)
        if d == 0:
            returned[e] = total.astype(bf16)
        elif d < ep_count:
            routed_done[d] = total.astype(bf16)
            send(
                routed_done.at[d],
                returned.at[e],
                back_z_send.at[d],
                back_z_recv.at[e],
                {"ep": source_of(d)},
            )
        elif d == ep_count:
            shared_sum[...] = total
        else:
            mixed_sum[...] = total.astype(bf16)

    last = ep_count - 1
    own[2].wait()
    for d in range(1, ep_count):
        landed(kv_all.at[source_of(d)], kv_recv.at[source_of(d)])
    pair_count = query.shape[0] // 2
    for n in range(pair_count):
        attend_two(n)
        if n == 0:
            pass_on(0)
    pass_on(ep_count)
    loads[0].wait()

    def expert_item(d):
        all_here(d)
        if d == 0:
            own[0].wait()
            for copy in loads[1:]:
                copy.wait()
        experts(d)
        to_sibling(d)

    for d in range(1, ep_count):
        come(d)
        if d == 1:
            project()
            to_sibling(ep_count + 1)
        else:
            pass_on(d - 1)
            expert_item(d - 2)
            if d == 2:
                all_here(ep_count)
                own[1].wait()
                share()
                to_sibling(ep_count)
            if d - 3 >= 1:
                across(d - 3)
    for d in range(1, last - 1):
        across(d)
    expert_item(last - 1)
    pass_on(last)
    across(last - 1)
    expert_item(last)
    for d in range(1, last - 1):
        finish(d)
    across(last)
    across(0)
    across(ep_count)
    across(ep_count + 1)
    for d in list(range(1, ep_count)) + [0, ep_count, ep_count + 1]:
        finish(d)
    for d in range(1, ep_count):
        landed(returned.at[source_of(d)], back_z_recv.at[source_of(d)])
    for copy in sends:
        copy.wait_send()


def whole(ep_count, tp_count, blocks, normed, kv, query, weights):
    local_count, capacity, width = blocks.shape[1:]
    vmem = pl.BlockSpec(memory_space=pltpu.VMEM)
    anywhere = pl.BlockSpec(memory_space=pl.ANY)
    half = tp_count // 2
    dma = pltpu.SemaphoreType.DMA
    block = (local_count, capacity, width)
    spread_block = (local_count, tp_count, ep_count, capacity, width)
    mixed = (query.shape[1] // tp_count, width)
    count = ep_count + 2

    def room(*shape):
        return pltpu.VMEM(shape, jnp.bfloat16)

    return pl.pallas_call(
        functools.partial(whole_kernel, ep_count, tp_count),
        out_shape=(
            jax.ShapeDtypeStruct((ep_count,) + block, jnp.bfloat16),
            jax.ShapeDtypeStruct(normed.shape, jnp.float32),
            jax.ShapeDtypeStruct(mixed, jnp.bfloat16),
        ),
        in_specs=[vmem] * 4 + [anywhere] * len(weights),
        out_specs=(vmem,) * 3,
        scratch_shapes=[
            room(*spread_block),
            room(tp_count, *normed.shape),
            room(ep_count, *kv.shape),
            *[room(*w.shape) for w in weights],
            room(query.shape[1], query.shape[0] // 2 * query.shape[2]),
            room(*spread_block),
            room(tp_count, *normed.shape),
            room(tp_count, *mixed),
            room(ep_count, half, *block),
            room(ep_count, half - 1, *block),
            room(ep_count, half - 1, *block),
            room(ep_count, *block),
            room(half, *normed.shape),
            room(half - 1, *normed.shape),
            room(half - 1, *normed.shape),
            room(half, *mixed),
            room(half - 1, *mixed),
            room(half - 1, *mixed),
            dma((3 + len(weights),)),
            dma((ep_count,)),
            dma((ep_count,)),
            dma((ep_count,)),
            dma((ep_count,)),
            dma((half, ep_count + 1)),
            dma((half, ep_count + 1)),
            dma((half, ep_count + 1)),
            dma((half, ep_count + 1)),
            dma((count, half)),
            dma((count, half)),
            dma((count, half)),
            dma((count, half)),
            dma((ep_count,)),
            dma((ep_count,)),
        ],
        compiler_params=pltpu.CompilerParams(
            collective_id=0, has_side_effects=True, vmem_limit_bytes=67043328
        ),
    )(blocks, normed, kv, query, *weights)


def body(
    queries,
    key_values,
    query_gain,
    key_gain,
    out_weight,
    second_batch,
    norm_gain,
    routes,
    route_weights,
    expert_gate,
    expert_up,
    expert_down,
    shared_gate,
    shared_up,
    shared_down,
):
    query_rows = queries.shape[0]
    head_size = query_gain.shape[0]
    heads_here = queries.shape[1] // head_size
    ep_count = lax.axis_size("ep")
    tp_count = lax.axis_size("tp")
    positions = lax.axis_index("ep") * query_rows + jnp.arange(query_rows, dtype=jnp.int32)
    query_turned = (
        turn_heads(
            head_norm(
                queries.reshape(query_rows, heads_here, head_size).astype(jnp.float32), query_gain
            ),
            positions,
        )
        * head_size ** (-0.5)
    ).astype(jnp.bfloat16)
    key_turned = turn_heads(
        head_norm(key_values[:, None, :head_size].astype(jnp.float32), key_gain), positions
    ).astype(jnp.bfloat16)
    keys_and_values = jnp.concatenate([key_turned[:, 0, :], key_values[:, head_size:]], axis=1)
    tok_count = second_batch.shape[0]
    model_width = second_batch.shape[1]
    top_count = routes.shape[1]
    local_experts = expert_gate.shape[0]
    expert_count = local_experts * ep_count
    capacity = 3 * tok_count * top_count // (2 * expert_count)
    capacity = (capacity + 7) // 8 * 8
    slot_count = expert_count * capacity
    token_float = second_batch.astype(jnp.float32)
    normed = (
        token_float
        * lax.rsqrt(jnp.mean(token_float * token_float, axis=-1, keepdims=True) + norm_eps)
        * norm_gain
    ).astype(jnp.bfloat16)
    own_slots = slot_ids(routes, expert_count, capacity)
    slot_numbers = jnp.arange(slot_count, dtype=jnp.int32)
    picks = [
        (own_slots[:, j][:, None] == slot_numbers[None, :]).astype(jnp.bfloat16)
        for j in range(top_count)
    ]
    outgoing = lax.dot_general(
        sum(picks), normed, (((0,), (0,)), ((), ())), preferred_element_type=jnp.float32
    ).astype(jnp.bfloat16)
    query_wide = jnp.pad(
        query_turned.transpose(1, 0, 2), ((0, 0), (0, 0), (0, key_values.shape[1] - head_size))
    )
    returned, shared_sum, mixer_out = whole(
        ep_count,
        tp_count,
        outgoing.reshape(ep_count, local_experts, capacity, model_width),
        normed,
        keys_and_values,
        query_wide,
        (
            out_weight,
            expert_gate,
            expert_up,
            expert_down,
            shared_gate,
            shared_up,
            shared_down,
        ),
    )
    returned = returned.reshape(slot_count, model_width)
    combined = shared_sum
    for j in range(top_count):
        combined = combined + route_weights[:, j : j + 1] * jnp.dot(
            picks[j], returned, preferred_element_type=jnp.float32
        )
    return (mixer_out, combined.astype(jnp.bfloat16))


def solution(mesh):
    placed = (
        P(("grp", "ep"), "tp"),
        P(("grp", "ep"), "tp"),
        P(),
        P(),
        P("tp", None),
        P(("grp", "ep", "tp"), None),
        P(),
        P(("grp", "ep", "tp"), None),
        P(("grp", "ep", "tp"), None),
        P("ep", None, "tp"),
        P("ep", None, "tp"),
        P("ep", "tp", None),
        P(None, "tp"),
        P(None, "tp"),
        P("tp", None),
    )
    return jax.shard_map(
        body,
        mesh=mesh,
        in_specs=placed,
        out_specs=(P(("grp", "ep", "tp"), None), P(("grp", "ep", "tp"), None)),
        check_vma=False,
    )
```

```python
import functools

import jax
import jax.numpy as jnp
from jax import lax
from jax.experimental import pallas as pl
from jax.experimental.pallas import tpu as pltpu
from jax.sharding import PartitionSpec as P

GRID_W = 64


rope_base = 10000.0
norm_eps = 1e-06


def head_norm(vectors, gain):
    return (
        vectors * lax.rsqrt(jnp.mean(vectors * vectors, axis=-1, keepdims=True) + norm_eps) * gain
    )


def turn_heads(vectors, positions):
    row_count, head_count, head_size = vectors.shape
    half_size = head_size // 2
    inverse = rope_base ** (-jnp.arange(0, half_size, 2, dtype=jnp.float32) / half_size)
    grid_row = (positions // GRID_W).astype(jnp.float32)
    grid_column = (positions % GRID_W).astype(jnp.float32)
    angles = jnp.concatenate([grid_row[:, None] * inverse, grid_column[:, None] * inverse], axis=-1)
    cosine = jnp.cos(angles)[:, None, :]
    sine = jnp.sin(angles)[:, None, :]
    paired = vectors.reshape(row_count, head_count, half_size, 2)
    first = paired[..., 0]
    second = paired[..., 1]
    turned = jnp.stack([first * cosine - second * sine, first * sine + second * cosine], axis=-1)
    return turned.reshape(vectors.shape)


def slot_ids(route_rows, expert_count, capacity):
    row_count, top_count = route_rows.shape
    flat_routes = route_rows.reshape(-1)
    pair_count = row_count * top_count
    onehot = flat_routes[:, None] == jnp.arange(expert_count, dtype=jnp.int32)[None, :]
    order = jnp.arange(pair_count, dtype=jnp.int32)
    before = (order[None, :] < order[:, None]).astype(jnp.bfloat16)
    earlier = jnp.dot(before, onehot.astype(jnp.bfloat16), preferred_element_type=jnp.float32)
    within = jnp.sum(jnp.where(onehot, earlier, 0.0), axis=1).astype(jnp.int32)
    return (flat_routes * capacity + within).reshape(row_count, top_count)


MESH = pl.DeviceIdType.MESH


def greet(ep_count, tp_count, e, t):
    barrier = pltpu.get_barrier_semaphore()
    peers = 0
    for d in range(1, ep_count):
        pl.semaphore_signal(
            barrier, inc=1, device_id={"ep": lax.rem(e + d, ep_count)}, device_id_type=MESH
        )
        peers += 1
    pair = t // 2
    core = lax.rem(t, 2)
    for k in range(1, tp_count // 2):
        pl.semaphore_signal(
            barrier,
            inc=1,
            device_id={"tp": lax.rem(pair + k, tp_count // 2) * 2 + core},
            device_id_type=MESH,
        )
        peers += 1
    pl.semaphore_signal(
        barrier, inc=1, device_id={"tp": pair * 2 + 1 - core}, device_id_type=MESH
    )
    peers += 1
    pl.semaphore_wait(barrier, peers)


def remote(src, dst, send, recv, device):
    return pltpu.make_async_remote_copy(
        src_ref=src,
        dst_ref=dst,
        send_sem=send,
        recv_sem=recv,
        device_id=device,
        device_id_type=MESH,
    )


def whole_kernel(
    ep_count,
    tp_count,
    blocks,
    normed,
    kv,
    query,
    picking,
    out_weight_hbm,
    gate_hbm,
    up_hbm,
    down_hbm,
    shared_gate_hbm,
    shared_up_hbm,
    shared_down_hbm,
    returned,
    shared_sum,
    mixed_sum,
    arrived,
    normed_all,
    kv_all,
    picking_all,
    out_weight,
    gate,
    up,
    down,
    shared_gate,
    shared_up,
    shared_down,
    heads_scr,
    routed,
    shared,
    mixed,
    routed_pair,
    routed_out,
    routed_in,
    routed_done,
    shared_pair,
    shared_out,
    shared_in,
    mixed_pair,
    mixed_out,
    mixed_in,
    local_sem,
    kv_send,
    kv_recv,
    z_send,
    z_recv,
    x_send,
    x_recv,
    d_send,
    d_recv,
    back_d_send,
    back_d_recv,
    back_x_send,
    back_x_recv,
    back_z_send,
    back_z_recv,
):
    e = lax.axis_index("ep")
    t = lax.axis_index("tp")
    half = tp_count // 2
    pair = t // 2
    core = lax.rem(t, 2)
    sibling = {"tp": pair * 2 + 1 - core}
    f32 = jnp.float32
    bf16 = jnp.bfloat16
    loads = [
        pltpu.make_async_copy(source, target, local_sem.at[3 + n])
        for n, (source, target) in enumerate(
            (
                (out_weight_hbm, out_weight),
                (gate_hbm, gate),
                (up_hbm, up),
                (down_hbm, down),
                (shared_gate_hbm, shared_gate),
                (shared_up_hbm, shared_up),
                (shared_down_hbm, shared_down),
            )
        )
    ]
    for copy in loads:
        copy.start()
    greet(ep_count, tp_count, e, t)

    sends = []

    def send(src, dst, send_sem, recv_sem, device):
        copy = remote(src, dst, send_sem, recv_sem, device)
        copy.start()
        sends.append(copy)

    def landed(spot, recv_sem):
        remote(spot, spot, kv_send.at[0], recv_sem, sibling).wait_recv()

    def source_of(d):
        return lax.rem(e - d + ep_count, ep_count)

    def place(d, row):
        if d == ep_count:
            return normed_all.at[row]
        if d == ep_count + 1:
            return picking_all.at[row]
        return arrived.at[:, row, source_of(d)]

    for d in range(1, ep_count):
        there = lax.rem(e + d, ep_count)
        send(kv, kv_all.at[e], kv_send.at[d], kv_recv.at[e], {"ep": there})
    for d in range(1, ep_count):
        there = lax.rem(e + d, ep_count)
        send(blocks.at[there], arrived.at[:, t, e], z_send.at[d], z_recv.at[e], {"ep": there})

    def spread(src, d):
        for k in range(1, half):
            other = lax.rem(pair + k, half)
            send(
                src,
                place(d, t),
                x_send.at[k, d],
                x_recv.at[pair, d],
                {"tp": other * 2 + core},
            )
        send(src, place(d, t), d_send.at[0, d], d_recv.at[pair, d], sibling)

    def pass_on(d):
        for k in range(1, half):
            other = lax.rem(pair + k, half)
            spot = place(d, other * 2 + core)
            landed(spot, x_recv.at[other, d])
            send(spot, spot, d_send.at[k, d], d_recv.at[other, d], sibling)

    def come(d):
        spot = arrived.at[:, t, source_of(d)]
        landed(spot, z_recv.at[source_of(d)])
        spread(spot, d)

    def all_here(d):
        for other in range(half):
            landed(place(d, other * 2 + 1 - core), d_recv.at[other, d])

    spread(picking, ep_count + 1)
    spread(normed, ep_count)
    own = [
        pltpu.make_async_copy(picking, picking_all.at[t], local_sem.at[0]),
        pltpu.make_async_copy(normed, normed_all.at[t], local_sem.at[1]),
        pltpu.make_async_copy(kv, kv_all.at[e], local_sem.at[2]),
    ]
    for copy in own:
        copy.start()

    query_rows, wide = query.shape[1], query.shape[2]
    model_width = normed.shape[1]
    tile = min(512, model_width)

    def attend(h):
        def step(b, carried):
            top_now, total_now, acc_now = carried
            block = kv_all[b]
            scores = lax.dot_general(
                query[h], block, (((1,), (1,)), ((), ())), preferred_element_type=f32
            )
            top_new = jnp.maximum(top_now, jnp.max(scores, axis=-1, keepdims=True))
            shrink = jnp.exp(top_now - top_new)
            exps = jnp.exp(scores - top_new)
            total_new = total_now * shrink + jnp.sum(exps, axis=-1, keepdims=True)
            acc_new = acc_now * shrink + jnp.dot(
                exps.astype(bf16), block, preferred_element_type=f32
            )
            return (top_new, total_new, acc_new)

        start = (
            jnp.full((query_rows, 1), -1e30, f32),
            jnp.zeros((query_rows, 1), f32),
            jnp.zeros((query_rows, wide), f32),
        )
        top, total, acc = lax.fori_loop(0, ep_count, step, start)
        return acc / total

    def attend_two(n):
        low = pltpu.roll(attend(2 * n), wide // 2, 1)
        high = attend(2 * n + 1)
        lane = lax.broadcasted_iota(jnp.int32, low.shape, 1)
        heads_scr[:, n * wide : (n + 1) * wide] = jnp.where(lane < wide // 2, low, high).astype(
            bf16
        )

    def project():
        def step(n, ignored):
            columns = pl.ds(pl.multiple_of(n * tile, tile), tile)
            part = jnp.dot(heads_scr[...], out_weight[:, columns], preferred_element_type=f32)
            mixed[:, :, columns] = part.astype(bf16).reshape(
                tp_count, query_rows // tp_count, tile
            )
            return ignored

        lax.fori_loop(0, model_width // tile, step, 0)

    local_count, capacity = arrived.shape[0], arrived.shape[3]

    def share():
        def step(row, ignored):
            rows = normed_all[row]
            gate_part = jnp.dot(rows, shared_gate[...], preferred_element_type=f32)
            up_part = jnp.dot(rows, shared_up[...], preferred_element_type=f32)
            hidden = (gate_part / (1.0 + jnp.exp(-gate_part)) * up_part).astype(bf16)
            weight = picking_all[row, 1]
            weight_high = weight.astype(bf16)
            weight_low = (weight - weight_high.astype(f32)).astype(bf16)

            def columns_step(m, inner):
                columns = pl.ds(pl.multiple_of(m * tile, tile), tile)
                results = routed[:, row, e, :, columns]
                if capacity % 16:
                    results = results.astype(f32)
                results = results.reshape(local_count * capacity, tile).astype(bf16)
                part = jnp.dot(hidden, shared_down[:, columns], preferred_element_type=f32)
                part = part + jnp.dot(weight_high, results, preferred_element_type=f32)
                part = part + jnp.dot(weight_low, results, preferred_element_type=f32)
                shared[row, :, columns] = part.astype(bf16)
                return inner

            lax.fori_loop(0, model_width // tile, columns_step, 0)
            return ignored

        lax.fori_loop(0, tp_count, step, 0)

    def pick_own():
        def step(row, ignored):
            chosen = picking_all[row, 0].astype(bf16)

            def columns_step(m, inner):
                columns = pl.ds(pl.multiple_of(m * tile, tile), tile)
                part = lax.dot_general(
                    chosen,
                    normed_all[row, :, columns],
                    (((0,), (0,)), ((), ())),
                    preferred_element_type=f32,
                )
                arrived[:, row, e, :, columns] = part.reshape(local_count, capacity, tile).astype(
                    bf16
                )
                return inner

            lax.fori_loop(0, model_width // tile, columns_step, 0)
            return ignored

        lax.fori_loop(0, tp_count, step, 0)

    def experts(d):
        source = source_of(d)

        def step(n, ignored):
            rows = arrived[n, :, source]
            if capacity % 16:
                rows = rows.astype(f32)
            rows = rows.reshape(tp_count * capacity, model_width).astype(bf16)
            gate_part = jnp.dot(rows, gate[n], preferred_element_type=f32)
            up_part = jnp.dot(rows, up[n], preferred_element_type=f32)
            hidden = (gate_part / (1.0 + jnp.exp(-gate_part)) * up_part).astype(bf16)

            def columns_step(m, inner):
                columns = pl.ds(pl.multiple_of(m * tile, tile), tile)
                part = jnp.dot(hidden, down[n, :, columns], preferred_element_type=f32)
                if capacity % 16:
                    part = part.reshape(tp_count, capacity, tile).astype(bf16)
                else:
                    part = part.astype(bf16).reshape(tp_count, capacity, tile)
                routed[n, :, source, :, columns] = part
                return inner

            lax.fori_loop(0, model_width // tile, columns_step, 0)
            return ignored

        lax.fori_loop(0, local_count, step, 0)

    def item(d):
        if d < ep_count:
            source = source_of(d)
            return (
                lambda row: routed.at[:, row, source],
                lambda k: routed_pair.at[d, k],
                lambda k: routed_out.at[d, k - 1],
                lambda k: routed_in.at[d, k - 1],
            )
        if d == ep_count:
            return (
                lambda row: shared.at[row],
                lambda k: shared_pair.at[k],
                lambda k: shared_out.at[k - 1],
                lambda k: shared_in.at[k - 1],
            )
        return (
            lambda row: mixed.at[row],
            lambda k: mixed_pair.at[k],
            lambda k: mixed_out.at[k - 1],
            lambda k: mixed_in.at[k - 1],
        )

    def to_sibling(d):
        part, paired, out, into = item(d)
        for k in list(range(1, half)) + [0]:
            other = lax.rem(pair + k, half)
            send(
                part(other * 2 + 1 - core),
                paired(k),
                back_d_send.at[d, k],
                back_d_recv.at[d, k],
                sibling,
            )

    def both(d, k):
        part, paired, out, into = item(d)
        spot = paired(k)
        landed(spot, back_d_recv.at[d, k])
        mine = part(lax.rem(pair + k, half) * 2 + core)
        return mine[...].astype(f32) + spot[...].astype(f32)

    crossed = set()

    def across(d):
        if d in crossed:
            return
        crossed.add(d)
        part, paired, out, into = item(d)
        for k in range(1, half):
            other = lax.rem(pair + k, half)
            out(k)[...] = both(d, k).astype(bf16)
            send(
                out(k),
                into(k),
                back_x_send.at[d, k],
                back_x_recv.at[d, k],
                {"tp": other * 2 + core},
            )

    finished = set()

    def finish(d):
        if d in finished:
            return
        finished.add(d)
        part, paired, out, into = item(d)
        total = both(d, 0)
        for k in range(1, half):
            spot = into(k)
            landed(spot, back_x_recv.at[d, k])
            total = total + spot[...].astype(f32)
        if d < ep_count:
            routed_done[d] = total.astype(bf16)
            send(
                routed_done.at[d],
                returned.at[e],
                back_z_send.at[d],
                back_z_recv.at[e],
                {"ep": source_of(d)},
            )
        elif d == ep_count:
            shared_sum[...] = total
        else:
            mixed_sum[...] = total.astype(bf16)

    last = ep_count - 1
    own[2].wait()
    for d in range(1, ep_count):
        landed(kv_all.at[source_of(d)], kv_recv.at[source_of(d)])
    pair_count = query.shape[0] // 2
    for n in range(pair_count):
        attend_two(n)
    pass_on(ep_count + 1)
    pass_on(ep_count)
    loads[0].wait()

    def expert_item(d):
        if d == 0:
            all_here(ep_count + 1)
            all_here(ep_count)
            own[0].wait()
            own[1].wait()
            pick_own()
            for copy in loads[1:]:
                copy.wait()
            experts(0)
            share()
            to_sibling(ep_count)
            returned[e] = jnp.zeros(returned.shape[1:], bf16)
            return
        all_here(d)
        experts(d)
        to_sibling(d)

    for d in range(1, ep_count):
        come(d)
        if d == 1:
            project()
            to_sibling(ep_count + 1)
        else:
            pass_on(d - 1)
            if d == 2:
                across(ep_count + 1)
            expert_item(d - 2)
            if d - 3 >= 1:
                across(d - 3)
    for d in range(1, last - 1):
        across(d)
    expert_item(last - 1)
    pass_on(last)
    across(last - 1)
    expert_item(last)
    for d in range(1, last - 1):
        finish(d)
    across(last)
    across(ep_count)
    across(ep_count + 1)
    for d in list(range(1, ep_count)) + [ep_count, ep_count + 1]:
        finish(d)
    for d in range(1, ep_count):
        landed(returned.at[source_of(d)], back_z_recv.at[source_of(d)])
    for copy in sends:
        copy.wait_send()


def whole(ep_count, tp_count, blocks, normed, kv, query, picking, weights):
    local_count, capacity, width = blocks.shape[1:]
    vmem = pl.BlockSpec(memory_space=pltpu.VMEM)
    anywhere = pl.BlockSpec(memory_space=pl.ANY)
    half = tp_count // 2
    dma = pltpu.SemaphoreType.DMA
    block = (local_count, capacity, width)
    spread_block = (local_count, tp_count, ep_count, capacity, width)
    mixed = (query.shape[1] // tp_count, width)
    count = ep_count + 2

    def room(*shape):
        return pltpu.VMEM(shape, jnp.bfloat16)

    return pl.pallas_call(
        functools.partial(whole_kernel, ep_count, tp_count),
        out_shape=(
            jax.ShapeDtypeStruct((ep_count,) + block, jnp.bfloat16),
            jax.ShapeDtypeStruct(normed.shape, jnp.float32),
            jax.ShapeDtypeStruct(mixed, jnp.bfloat16),
        ),
        in_specs=[vmem] * 5 + [anywhere] * len(weights),
        out_specs=(vmem,) * 3,
        scratch_shapes=[
            room(*spread_block),
            room(tp_count, *normed.shape),
            room(ep_count, *kv.shape),
            pltpu.VMEM((tp_count,) + picking.shape, jnp.float32),
            *[room(*w.shape) for w in weights],
            room(query.shape[1], query.shape[0] // 2 * query.shape[2]),
            room(*spread_block),
            room(tp_count, *normed.shape),
            room(tp_count, *mixed),
            room(ep_count, half, *block),
            room(ep_count, half - 1, *block),
            room(ep_count, half - 1, *block),
            room(ep_count, *block),
            room(half, *normed.shape),
            room(half - 1, *normed.shape),
            room(half - 1, *normed.shape),
            room(half, *mixed),
            room(half - 1, *mixed),
            room(half - 1, *mixed),
            dma((3 + len(weights),)),
            dma((ep_count,)),
            dma((ep_count,)),
            dma((ep_count,)),
            dma((ep_count,)),
            dma((half, ep_count + 2)),
            dma((half, ep_count + 2)),
            dma((half, ep_count + 2)),
            dma((half, ep_count + 2)),
            dma((count, half)),
            dma((count, half)),
            dma((count, half)),
            dma((count, half)),
            dma((ep_count,)),
            dma((ep_count,)),
        ],
        compiler_params=pltpu.CompilerParams(
            collective_id=0, has_side_effects=True, vmem_limit_bytes=67043328
        ),
    )(blocks, normed, kv, query, picking, *weights)


def body(
    queries,
    key_values,
    query_gain,
    key_gain,
    out_weight,
    second_batch,
    norm_gain,
    routes,
    route_weights,
    expert_gate,
    expert_up,
    expert_down,
    shared_gate,
    shared_up,
    shared_down,
):
    query_rows = queries.shape[0]
    head_size = query_gain.shape[0]
    heads_here = queries.shape[1] // head_size
    ep_count = lax.axis_size("ep")
    tp_count = lax.axis_size("tp")
    positions = lax.axis_index("ep") * query_rows + jnp.arange(query_rows, dtype=jnp.int32)
    query_turned = (
        turn_heads(
            head_norm(
                queries.reshape(query_rows, heads_here, head_size).astype(jnp.float32), query_gain
            ),
            positions,
        )
        * head_size ** (-0.5)
    ).astype(jnp.bfloat16)
    key_turned = turn_heads(
        head_norm(key_values[:, None, :head_size].astype(jnp.float32), key_gain), positions
    ).astype(jnp.bfloat16)
    keys_and_values = jnp.concatenate([key_turned[:, 0, :], key_values[:, head_size:]], axis=1)
    tok_count = second_batch.shape[0]
    model_width = second_batch.shape[1]
    top_count = routes.shape[1]
    local_experts = expert_gate.shape[0]
    expert_count = local_experts * ep_count
    capacity = 3 * tok_count * top_count // (2 * expert_count)
    capacity = (capacity + 7) // 8 * 8
    slot_count = expert_count * capacity
    token_float = second_batch.astype(jnp.float32)
    normed = (
        token_float
        * lax.rsqrt(jnp.mean(token_float * token_float, axis=-1, keepdims=True) + norm_eps)
        * norm_gain
    ).astype(jnp.bfloat16)
    own_slots = slot_ids(routes, expert_count, capacity)
    slot_numbers = jnp.arange(slot_count, dtype=jnp.int32)
    picks = [
        (own_slots[:, j][:, None] == slot_numbers[None, :]).astype(jnp.bfloat16)
        for j in range(top_count)
    ]
    outgoing = lax.dot_general(
        sum(picks), normed, (((0,), (0,)), ((), ())), preferred_element_type=jnp.float32
    ).astype(jnp.bfloat16)
    near_count = local_experts * capacity
    near_slots = lax.axis_index("ep") * near_count + jnp.arange(near_count, dtype=jnp.int32)
    near = [own_slots[:, j][:, None] == near_slots[None, :] for j in range(top_count)]
    picking = jnp.stack(
        [
            sum(jnp.where(match, 1.0, 0.0) for match in near),
            sum(
                jnp.where(match, route_weights[:, j : j + 1], 0.0) for j, match in enumerate(near)
            ),
        ]
    )
    query_wide = jnp.pad(
        query_turned.transpose(1, 0, 2), ((0, 0), (0, 0), (0, key_values.shape[1] - head_size))
    )
    returned, shared_sum, mixer_out = whole(
        ep_count,
        tp_count,
        outgoing.reshape(ep_count, local_experts, capacity, model_width),
        normed,
        keys_and_values,
        query_wide,
        picking,
        (
            out_weight,
            expert_gate,
            expert_up,
            expert_down,
            shared_gate,
            shared_up,
            shared_down,
        ),
    )
    returned = returned.reshape(slot_count, model_width)
    combined = shared_sum
    for j in range(top_count):
        combined = combined + route_weights[:, j : j + 1] * jnp.dot(
            picks[j], returned, preferred_element_type=jnp.float32
        )
    return (mixer_out, combined.astype(jnp.bfloat16))


def solution(mesh):
    placed = (
        P(("grp", "ep"), "tp"),
        P(("grp", "ep"), "tp"),
        P(),
        P(),
        P("tp", None),
        P(("grp", "ep", "tp"), None),
        P(),
        P(("grp", "ep", "tp"), None),
        P(("grp", "ep", "tp"), None),
        P("ep", None, "tp"),
        P("ep", None, "tp"),
        P("ep", "tp", None),
        P(None, "tp"),
        P(None, "tp"),
        P("tp", None),
    )
    return jax.shard_map(
        body,
        mesh=mesh,
        in_specs=placed,
        out_specs=(P(("grp", "ep", "tp"), None), P(("grp", "ep", "tp"), None)),
        check_vma=False,
    )
```
